32 devices in a mesh: ep: 4 (over y, x), tp: 8 (over z, core).
Axes of the slice: x: 2, y: 2, z: 4, core: 2. Of those that a mesh axis runs over, the one named last changes fastest.
Arguments:
- tokens: bfloat16 [512, 2048], P('ep'), may hold values from -32 to 32
- routes: int32 [512, 2], P('ep'), may hold values from 0 to 3, all different within a row; in each aligned block of 128 rows (0 to 127, 128 to 255, ...) at most 96 rows name the same one
- gates: float32 [512, 2], P('ep'), may hold values from 0.05 to 0.6
- cotangent: bfloat16 [512, 2048], P('ep'), may hold values from -6 to 6
- w_glu: bfloat16 [4, 2048, 1024], P('ep', None, 'tp'), may hold values from -0.125 to 0.125
- w_lin: bfloat16 [4, 2048, 1024], P('ep', None, 'tp'), may hold values from -0.125 to 0.125
- w_down: bfloat16 [4, 1024, 2048], P('ep', 'tp'), may hold values from -0.1875 to 0.1875
Outputs:
- d_tokens: bfloat16 [512, 2048], P('ep', 'tp')
- d_gates: float32 [512, 2], P('ep')
- glu_wgrad: float32 [4, 2048, 1024], P('ep', None, 'tp')
- lin_wgrad: float32 [4, 2048, 1024], P('ep', None, 'tp')
- down_wgrad: float32 [4, 1024, 2048], P('ep', 'tp')
- glu_norms: float32 [4, 2048], P('ep')
- lin_norms: float32 [4, 2048], P('ep')
- down_norms: float32 [4, 1024], P('ep', 'tp')
The draws below stay inside these ranges and needn't reach their ends.
Inputs may be any that keep to these rules, and one draw needn't show every extreme that they name: `routes`: each row names 2 different experts. Among the 128 tokens of one aligned block no expert is named more than 96 times, and in every draw some expert is named exactly 96 times in some block.
All inputs are finite; a program needn't handle non-finite values.
Results may differ from the reference program's by a relative error of at most 0.024.
Values may be sent and summed in bfloat16 or wider, within the bound.
A program may use at most 64 MiB of HBM per device.

```python
import math
import jax
import jax.numpy as jnp
import numpy as np
from jax import lax

D = 2048
F = 1024
TOP = 2
TOK_DEV = 128
EXPERTS = 4
CAP = 96
TOKENS = 512
N_EP = 4
N_TP = 8


def draw_tokens(key, part):
    first_key, second_key, third_key = jax.random.split(key, 3)
    values = jnp.clip(jax.random.normal(first_key, (TOKENS, D), jnp.float32), -4.0, 4.0)
    return values.astype(jnp.bfloat16)


def steps_of(key, extent, cuts, least, largest):
    loudness = 1.0
    for axis_at, shards_of in cuts:
        steps = jax.random.uniform(jax.random.fold_in(jax.random.fold_in(key, 6), axis_at), (shards_of,), jnp.float32, least / len(cuts), largest / len(cuts))
        loudness = loudness * jnp.repeat(jnp.exp(steps), extent[axis_at] // shards_of).reshape((-1,) + (1,) * (len(extent) - 1 - axis_at))
    return loudness


def routed_block(own_key, own, number, rows, number_of, top, reach, slope):
    sequence = jax.random.permutation(own_key, number_of)
    packed, common = portions_of(number_of, rows * top, reach, slope, True), portions_of(number_of, rows * top, reach, slope, False)
    places = jnp.arange(number_of)

    def named(sizes, turn):
        used = int((sizes > 0).sum())
        fixed = max(1, used // 4)
        shifted = fixed + (places - fixed + turn * (used - fixed)) % max(1, number_of - fixed)
        return jnp.zeros((number_of,), jnp.int32).at[sequence[jnp.where(places < fixed, places, shifted)]].set(jnp.asarray(sizes, jnp.int32))

    sizes = jnp.where(number % 4 == 0, named(packed, number // 4), named(common, number - number // 4 - 1))
    mixed = jax.random.permutation(jax.random.fold_in(own, 3), number_of)
    source_of, sink = mixed[0:number_of // 2 * 2:2], mixed[1:number_of // 2 * 2:2]
    margin = jnp.minimum(sizes[source_of] - 1, reach - sizes[sink]) // 2
    margin = jnp.where((source_of == sequence[0]) | (sink == sequence[0]) | (sizes[sink] == 0), 0, jnp.maximum(margin, 0))
    shifted = jax.random.randint(jax.random.fold_in(own, 4), (number_of // 2,), 0, 1 << 20) % (margin + 1)
    sizes = sizes.at[source_of].add(-shifted).at[sink].add(shifted)
    members = jnp.searchsorted(jnp.cumsum(sizes), jnp.arange(rows * top), side="right").astype(jnp.int32)
    listing = members.reshape(top, rows).T
    listing = listing[jax.random.permutation(jax.random.fold_in(own, 1), rows)]
    turn = jax.random.randint(jax.random.fold_in(own, 2), (rows, 1), 0, top)
    return jnp.take_along_axis(listing, (jnp.arange(top)[None, :] + turn) % top, axis=1)


def portions_of(count, total, most, lean, full):
    portions = [(1 << 20) // math.isqrt(grade ** lean) + 1 for grade in range(1, count + 1)]
    largest = most if full else min(most, max(-(-total // count), total * portions[0] // sum(portions)))
    least = 1 if total - largest >= count - 1 else 0
    counts, spare = [largest] + [least] * (count - 1), total - largest - least * (count - 1)
    while spare > 0:
        candidates = [i for i in range(1, count) if counts[i] < largest] or [i for i in range(1, count) if counts[i] < most]
        mass, left = sum([portions[i] for i in candidates]), spare
        for i in candidates:
            addition = min(most - counts[i], max(1, left * portions[i] // mass), spare)
            counts[i] = counts[i] + addition
            spare = spare - addition
    return np.array(counts)


def normal_values(own_key, dims, deviation, bound, shards=(), kind=jnp.bfloat16):
    array = deviation * jax.random.normal(own_key, dims, jnp.float32)
    if shards:
        array = array * steps_of(own_key, dims, shards, -0.22, 0.18)
    return jnp.clip(array, -bound, bound).astype(kind)


def setup_inputs(seed: int = 0) -> dict:
    streams_of = jax.random.split(jax.random.key(seed), 8)
    tokens = draw_tokens(jax.random.fold_in(streams_of[7], 71), 0)
    routes_keys = jax.random.split(jax.random.fold_in(streams_of[1], 1), TOKENS // TOK_DEV)
    routes_turns = jax.random.permutation(jax.random.fold_in(streams_of[1], 3), TOKENS // TOK_DEV)
    routes = jax.vmap(lambda own, number: routed_block(jax.random.fold_in(streams_of[1], 2), own, number, TOK_DEV, EXPERTS, TOP, CAP, 2))(routes_keys, routes_turns).reshape((TOKENS, TOP))
    gates = jnp.clip(jnp.exp(math.log(0.6) - 2.4849067 * jax.random.uniform(streams_of[2], (TOKENS, TOP), jnp.float32) ** steps_of(streams_of[2], (TOKENS, TOP), ((0, 4),), -0.2, 0.2)), 0.05, 0.6)
    cotangent = normal_values(streams_of[3], (TOKENS, D), 1.0, 6.0, ((0, 4),))
    w_glu = normal_values(streams_of[4], (EXPERTS, D, F), D ** -0.5, 0.125, ((0, 4), (2, 8)))
    w_lin = normal_values(streams_of[5], (EXPERTS, D, F), D ** -0.5, 0.125, ((0, 4), (2, 8)))
    w_down = normal_values(streams_of[6], (EXPERTS, F, D), F ** -0.5, 0.1875, ((0, 4), (1, 8)))
    return {"tokens": tokens, "routes": routes, "gates": gates, "cotangent": cotangent, "w_glu": w_glu, "w_lin": w_lin, "w_down": w_down}


clamp_limit = 7.0
sigmoid_scale = 1.702


def slot_rank(pair_expert, all_experts):
    onehot = (pair_expert[:, None] == jnp.arange(all_experts, dtype=jnp.int32)[None, :]).astype(jnp.int32)
    return (jnp.sum(jnp.cumsum(onehot, axis=0) * onehot, axis=1) - 1).astype(jnp.int32)


def clamp_backward(glu_pre, lin_pre, back_proj, gate_col):
    glu_clip = jnp.minimum(glu_pre, clamp_limit)
    lin_clip = jnp.clip(lin_pre, -clamp_limit, clamp_limit)
    sig_val = jax.nn.sigmoid(sigmoid_scale * glu_clip)
    glu_act = glu_clip * sig_val
    hidden = glu_act * (lin_clip + 1.0)
    hid_grad = gate_col * back_proj
    act_slope = sig_val + sigmoid_scale * glu_clip * sig_val * (1.0 - sig_val)
    glu_grad = jnp.where(glu_pre < clamp_limit, hid_grad * (lin_clip + 1.0) * act_slope, 0.0)
    lin_grad = jnp.where(jnp.abs(lin_pre) < clamp_limit, hid_grad * glu_act, 0.0)
    return hidden, glu_grad.astype(jnp.bfloat16), lin_grad.astype(jnp.bfloat16)


def expert_grads(tok_rows, cot_rows, gate_col, glu_w, lin_w, down_w):
    glu_pre = jnp.dot(tok_rows, glu_w, preferred_element_type=jnp.float32)
    lin_pre = jnp.dot(tok_rows, lin_w, preferred_element_type=jnp.float32)
    back_proj = jnp.dot(cot_rows, down_w.T, preferred_element_type=jnp.float32)
    hidden, glu_bf, lin_bf = clamp_backward(glu_pre, lin_pre, back_proj, gate_col)
    gate_part = jnp.sum(back_proj * hidden, axis=1)
    hidden_gated = (gate_col * hidden).astype(jnp.bfloat16)
    down_wgrad = jnp.dot(hidden_gated.T, cot_rows, preferred_element_type=jnp.float32)
    glu_wgrad = jnp.dot(tok_rows.T, glu_bf, preferred_element_type=jnp.float32)
    lin_wgrad = jnp.dot(tok_rows.T, lin_bf, preferred_element_type=jnp.float32)
    return gate_part, glu_bf, lin_bf, glu_wgrad, lin_wgrad, down_wgrad


def rank_block(block_row):
    return slot_rank(block_row, EXPERTS)


def reference(tokens, routes, gates, cotangent, w_glu, w_lin, w_down):
    pair_count = TOK_DEV * TOP
    slot_total = N_EP * CAP
    block_width = F // N_TP
    block_experts = routes.reshape(N_EP, pair_count)
    ranks = jax.vmap(rank_block)(block_experts)
    sources = jnp.arange(N_EP, dtype=jnp.int32)[:, None] * CAP
    slot_index = (block_experts * slot_total + sources + ranks).reshape(-1).astype(jnp.int32)
    slot_pair = jnp.full((EXPERTS * slot_total,), TOKENS * TOP, jnp.int32).at[slot_index].set(
        jnp.arange(TOKENS * TOP, dtype=jnp.int32)).reshape(EXPERTS, slot_total)
    slot_token = (slot_pair // TOP).astype(jnp.int32)
    tok_ext = jnp.concatenate([tokens, jnp.zeros((1, D), jnp.bfloat16)], axis=0)
    cot_ext = jnp.concatenate([cotangent, jnp.zeros((1, D), jnp.bfloat16)], axis=0)
    gate_ext = jnp.concatenate([gates.reshape(-1), jnp.zeros((1,), jnp.float32)])

    def one_expert(inputs):
        token_ids, pair_ids, glu_w, lin_w, down_w = inputs
        tok_rows = tok_ext[token_ids]
        cot_rows = cot_ext[token_ids]
        gate_col = gate_ext[pair_ids][:, None]
        gate_part, glu_bf, lin_bf, glu_wgrad, lin_wgrad, down_wgrad = expert_grads(
            tok_rows, cot_rows, gate_col, glu_w, lin_w, down_w)
        glu_blocks = glu_bf.reshape(slot_total, N_TP, block_width).transpose(1, 0, 2)
        lin_blocks = lin_bf.reshape(slot_total, N_TP, block_width).transpose(1, 0, 2)
        glu_wblocks = glu_w.reshape(D, N_TP, block_width).transpose(1, 0, 2)
        lin_wblocks = lin_w.reshape(D, N_TP, block_width).transpose(1, 0, 2)

        def add_block(total, pieces):
            glu_piece, lin_piece, glu_wpiece, lin_wpiece = pieces
            term = jnp.dot(glu_piece, glu_wpiece.T, preferred_element_type=jnp.float32)
            term = term + jnp.dot(lin_piece, lin_wpiece.T, preferred_element_type=jnp.float32)
            rounded = lax.optimization_barrier(term.astype(jnp.bfloat16))
            return total + rounded.astype(jnp.float32), None

        total, unused = lax.scan(add_block, jnp.zeros((slot_total, D), jnp.float32),
                                 (glu_blocks, lin_blocks, glu_wblocks, lin_wblocks))
        return total.astype(jnp.bfloat16), gate_part, glu_wgrad, lin_wgrad, down_wgrad

    slot_grads, gate_slots, glu_wgrad, lin_wgrad, down_wgrad = lax.map(
        one_expert, (slot_token, slot_pair, w_glu, w_lin, w_down))
    pair_grads = slot_grads.reshape(-1, D)[slot_index].astype(jnp.float32)
    d_tokens = jnp.sum(pair_grads.reshape(TOKENS, TOP, D), axis=1).astype(jnp.bfloat16)
    d_gates = gate_slots.reshape(-1)[slot_index].reshape(TOKENS, TOP)
    glu_norms = jnp.sum(glu_wgrad * glu_wgrad, axis=2)
    lin_norms = jnp.sum(lin_wgrad * lin_wgrad, axis=2)
    down_norms = jnp.sum(down_wgrad * down_wgrad, axis=2)
    return (d_tokens, d_gates, glu_wgrad, lin_wgrad, down_wgrad, glu_norms, lin_norms, down_norms)
```

```python
import functools

import jax
import jax.numpy as jnp
from jax import lax
from jax.experimental import pallas as pl
from jax.experimental.pallas import tpu as pltpu
from jax.sharding import PartitionSpec as P

clamp_limit = 7.0
sigmoid_scale = 1.702
MESH = pl.DeviceIdType.MESH
LANES = 128
CORES = 2
f32 = jnp.float32
bf16 = jnp.bfloat16


def dot_nn(a, b):
    return lax.dot_general(a, b, (((1,), (0,)), ((), ())), preferred_element_type=f32)


def dot_nt(a, b):
    return lax.dot_general(a, b, (((1,), (1,)), ((), ())), preferred_element_type=f32)


def clamp_backward(glu_pre, lin_pre, back_proj, gate_col):
    glu_clip = jnp.minimum(glu_pre, clamp_limit)
    lin_clip = jnp.clip(lin_pre, -clamp_limit, clamp_limit)
    sig_val = jax.nn.sigmoid(sigmoid_scale * glu_clip)
    glu_act = glu_clip * sig_val
    hidden = glu_act * (lin_clip + 1.0)
    hid_grad = gate_col * back_proj
    act_slope = sig_val + sigmoid_scale * glu_clip * sig_val * (1.0 - sig_val)
    glu_grad = jnp.where(glu_pre < clamp_limit, hid_grad * (lin_clip + 1.0) * act_slope, 0.0)
    lin_grad = jnp.where(jnp.abs(lin_pre) < clamp_limit, hid_grad * glu_act, 0.0)
    return hidden, glu_grad.astype(bf16), lin_grad.astype(bf16)


def kernel(
    ep, tp, cap,
    tok_ref, routes_ref, gates_ref, cot_ref, wg_ref, wl_ref, wd_ref,
    dtok_ref, dgate_ref, gw_ref, lw_ref, dw_ref, gn_ref, ln_ref, dn_ref,
    pt_v, snd_v, all_v, gsnd_v, grow_v, bf_v, tr_v,
    ps_v, pr_v, mine_v, xs_v, ret_v, zs_v, zr_v,
    gp_v, gsum_v, gback_v, ns_v, nr_v, gw_v, lw_v, dw_v,
    d_s, d_r, g_s, g_r, y_s, y_r, p_s, p_r, x_s, x_r, z_s, z_r,
    a_s, a_r, b_s, b_r, n_s, n_r, o_s,
):
    me = lax.axis_index("ep")
    tpi = lax.axis_index("tp")
    nz = tp // CORES
    core = lax.rem(tpi, CORES)
    chip = lax.div(tpi, CORES)
    other = 1 - core
    partner = chip * CORES + other
    rows = tok_ref.shape[0]
    width = tok_ref.shape[1]
    hidden_units = wg_ref.shape[1]
    half = width // CORES
    own = width // tp

    def ahead(r):
        return lax.rem(me + r, ep)

    def behind(r):
        return lax.rem(me + ep - r, ep)

    barrier = pltpu.get_barrier_semaphore()
    for r in range(1, ep):
        pl.semaphore_signal(barrier, inc=1, device_id={"ep": ahead(r)}, device_id_type=MESH)
    for q in range(1, tp):
        pl.semaphore_signal(
            barrier, inc=1, device_id={"tp": lax.rem(tpi + q, tp)}, device_id_type=MESH
        )

    def remote(src, dst, ss, rs, where):
        return pltpu.make_async_remote_copy(
            src_ref=src, dst_ref=dst, send_sem=ss, recv_sem=rs,
            device_id=where, device_id_type=MESH,
        )

    rel = routes_ref[...] - me
    rel = jnp.where(rel < 0, rel + ep, rel)
    lane = lax.broadcasted_iota(jnp.int32, (rows, LANES), 1)
    first, second = lane == rel[:, 0:1], lane == rel[:, 1:2]
    mask = jnp.where(first, 1.0, 0.0) + jnp.where(second, 1.0, 0.0)
    gate_of = jnp.where(first, gates_ref[:, 0:1], 0.0) + jnp.where(second, gates_ref[:, 1:2], 0.0)
    before = lax.broadcasted_iota(jnp.int32, (rows, rows), 1) < lax.broadcasted_iota(
        jnp.int32, (rows, rows), 0
    )
    rank = dot_nn(jnp.where(before, 1.0, 0.0).astype(bf16), mask.astype(bf16))
    place = jnp.where(mask > 0.5, rank, -1.0)
    lane_f = lane.astype(f32)
    sends = []
    picks = []
    for r in range(ep):
        hit = jnp.where(lane_f == place[:, r:r + 1], 1.0, 0.0)
        pt_v[r] = hit.astype(bf16)
        picks.append(hit.T[:cap, :].astype(bf16))
        row = jnp.sum(hit * gate_of[:, r:r + 1], axis=0, keepdims=True)
        if r == 0:
            grow_v[0] = jnp.broadcast_to(row, (8, LANES))
        else:
            gsnd_v[r] = jnp.broadcast_to(row, (8, LANES))
    half_cols = pl.ds(pl.multiple_of(core * half, half), half)
    waited = False
    for r in range(1, ep):
        for a, ref in ((0, tok_ref), (1, cot_ref)):
            snd_v[a, r] = dot_nn(picks[r], ref[:, half_cols]).astype(bf16)
            if not waited:
                pl.semaphore_wait(barrier, ep - 1 + tp - 1)
                waited = True
            cp = remote(
                snd_v.at[a, r], all_v.at[a, core, pl.ds(r * cap, cap), :],
                d_s.at[a, r], d_r.at[a, r], {"ep": ahead(r)},
            )
            cp.start()
            sends.append(cp)
        cp = remote(gsnd_v.at[r], grow_v.at[r], g_s.at[r], g_r.at[r], {"ep": ahead(r)})
        cp.start()
        sends.append(cp)
    for a, ref in ((0, tok_ref), (1, cot_ref)):
        for h in range(CORES):
            all_v[a, h, 0:cap, :] = dot_nn(picks[0], ref[:, h * half:(h + 1) * half]).astype(bf16)

    eye = lax.broadcasted_iota(jnp.int32, (cap, LANES), 0) == lax.broadcasted_iota(
        jnp.int32, (cap, LANES), 1
    )

    gp_v[tpi] = jnp.zeros(gp_v.shape[1:], f32)

    def forward(r):
        rs = slice(r * cap, (r + 1) * cap)
        glu_pre = jnp.zeros((cap, hidden_units), f32)
        lin_pre = glu_pre
        back = glu_pre
        for h in range(CORES):
            hs = slice(h * half, (h + 1) * half)
            glu_pre = glu_pre + dot_nn(all_v[0, h, rs, :], wg_ref[hs, :])
            lin_pre = lin_pre + dot_nn(all_v[0, h, rs, :], wl_ref[hs, :])
            back = back + dot_nt(all_v[1, h, rs, :], wd_ref[:, hs])
        gate_col = jnp.sum(jnp.where(eye, grow_v[r, 0:1, :], 0.0), axis=1, keepdims=True)
        hidden, glu_bf, lin_bf = clamp_backward(glu_pre, lin_pre, back, gate_col)
        part = jnp.sum(back * hidden, axis=1, keepdims=True)
        gp_v[tpi, r:r + 1, :] = jnp.sum(jnp.where(eye, part, 0.0), axis=0, keepdims=True)
        bf_v[0, rs, :] = glu_bf
        bf_v[1, rs, :] = lin_bf
        bf_v[2, rs, :] = (gate_col * hidden).astype(bf16)

    forward(0)
    relays = []
    for r in range(1, ep):
        for a in range(2):
            mine = all_v.at[a, core, pl.ds(r * cap, cap), :]
            remote(snd_v.at[a, r], mine, d_s.at[a, r], d_r.at[a, r], {"ep": ahead(r)}).wait_recv()
            cp = remote(mine, mine, y_s.at[a, r], y_r.at[a, r], {"tp": partner})
            cp.start()
            relays.append(cp)
    for r in range(1, ep):
        for a in range(2):
            theirs = all_v.at[a, other, pl.ds(r * cap, cap), :]
            remote(theirs, theirs, y_s.at[a, r], y_r.at[a, r], {"tp": partner}).wait_recv()
        remote(gsnd_v.at[r], grow_v.at[r], g_s.at[r], g_r.at[r], {"ep": ahead(r)}).wait_recv()
        forward(r)

    for q in range(1, tp):
        cp = remote(gp_v.at[tpi], gp_v.at[tpi], a_s.at[q], a_r.at[q], {"tp": lax.rem(tpi + q, tp)})
        cp.start()
        sends.append(cp)

    def input_cols(q, which):
        z = lax.rem(chip + q, nz)
        at = pl.ds(pl.multiple_of((z * CORES + which) * own, own), own)
        return dot_nt(bf_v[0], wg_ref[at, :]) + dot_nt(bf_v[1], wl_ref[at, :])

    order = list(range(1, nz)) + [0]
    for q in order:
        ps_v[q] = input_cols(q, other).astype(bf16)
        cp = remote(ps_v.at[q], pr_v.at[q], p_s.at[q], p_r.at[q], {"tp": partner})
        cp.start()
        sends.append(cp)
    for q in order:
        mine_v[q] = input_cols(q, core)
    for q in order:
        remote(ps_v.at[q], pr_v.at[q], p_s.at[q], p_r.at[q], {"tp": partner}).wait_recv()
        total = (mine_v[q] + pr_v[q].astype(f32)).astype(bf16)
        ret_v[q, 0:cap, :] = total[0:cap, :]
        for r in range(1, ep):
            rs = slice(r * cap, (r + 1) * cap)
            xs_v[q, rs, :] = total[rs, :]
        for r in range(1, ep):
            rs = pl.ds(r * cap, cap)
            cp = remote(
                xs_v.at[q, rs, :], ret_v.at[q, rs, :],
                x_s.at[q, r], x_r.at[q, r], {"ep": behind(r)},
            )
            cp.start()
            sends.append(cp)

    for i in range(3):
        tr_v[i] = bf_v[i].astype(f32).T.astype(bf16)
    step = min(512, half)
    outs = []
    for h in range(CORES):
        for c0 in range(0, half, step):
            cols = slice(h * half + c0, h * half + c0 + step)
            x = all_v[0, h, :, c0:c0 + step]
            for i, (w_v, at) in enumerate(((gw_v, 0), (lw_v, 1))):
                w = dot_nn(tr_v[i], x)
                ns_v[at:at + 1, cols] = jnp.sum(w * w, axis=0, keepdims=True)
                w_v[cols, :] = w.T
    nr_v[tpi] = ns_v[...]
    for q in range(1, tp):
        cp = remote(ns_v, nr_v.at[tpi], n_s.at[q], n_r.at[q], {"tp": lax.rem(tpi + q, tp)})
        cp.start()
        sends.append(cp)
    for i, (src, dst) in enumerate(((gw_v, gw_ref), (lw_v, lw_ref))):
        cp = pltpu.make_async_copy(src, dst, o_s.at[i])
        cp.start()
        outs.append(cp)

    for q in range(1, tp):
        frm = lax.rem(tpi + tp - q, tp)
        remote(gp_v.at[tpi], gp_v.at[frm], a_s.at[q], a_r.at[q], {"tp": partner}).wait_recv()
    gsum = gp_v[0]
    for j in range(1, tp):
        gsum = gsum + gp_v[j]
    gback_v[0, 0:1, :] = gsum[0:1, :]
    for r in range(1, ep):
        gsum_v[r] = jnp.broadcast_to(gsum[r:r + 1, :], (8, LANES))
        cp = remote(gsum_v.at[r], gback_v.at[r], b_s.at[r], b_r.at[r], {"ep": behind(r)})
        cp.start()
        sends.append(cp)

    norm = jnp.zeros((hidden_units, 1), f32)
    for h in range(CORES):
        for c0 in range(0, half, step):
            cols = slice(h * half + c0, h * half + c0 + step)
            w = dot_nn(tr_v[2], all_v[1, h, :, c0:c0 + step])
            norm = norm + jnp.sum(w * w, axis=1, keepdims=True)
            dw_v[:, cols] = w
    cp = pltpu.make_async_copy(dw_v, dw_ref, o_s.at[2])
    cp.start()
    outs.append(cp)
    diag = lax.broadcasted_iota(jnp.int32, (hidden_units, hidden_units), 0) == (
        lax.broadcasted_iota(jnp.int32, (hidden_units, hidden_units), 1)
    )
    dn_ref[...] = jnp.sum(jnp.where(diag, norm, 0.0), axis=0, keepdims=True)

    acc = None
    for q in order:
        part = None
        for r in range(ep):
            rs = pl.ds(r * cap, cap)
            if r > 0:
                remote(
                    xs_v.at[q, rs, :], ret_v.at[q, rs, :],
                    x_s.at[q, r], x_r.at[q, r], {"ep": behind(r)},
                ).wait_recv()
            term = dot_nn(pt_v[r][:, :cap], ret_v[q, r * cap:(r + 1) * cap, :])
            part = term if part is None else part + term
        if q == 0:
            acc = part
        else:
            zs_v[q] = part.astype(bf16)
            to = lax.rem(chip + q, nz) * CORES + core
            cp = remote(zs_v.at[q], zr_v.at[q], z_s.at[q], z_r.at[q], {"tp": to})
            cp.start()
            sends.append(cp)

    res = [jnp.zeros((rows, 1), f32), jnp.zeros((rows, 1), f32)]
    for r in range(ep):
        if r > 0:
            remote(
                gsum_v.at[r], gback_v.at[r], b_s.at[r], b_r.at[r], {"ep": behind(r)}
            ).wait_recv()
        val = jnp.sum(pt_v[r].astype(f32) * gback_v[r, 0:1, :], axis=1, keepdims=True)
        for k in range(2):
            res[k] = res[k] + jnp.where(rel[:, k:k + 1] == r, val, 0.0)
    dgate_ref[:, 0:1] = res[0]
    dgate_ref[:, 1:2] = res[1]

    for q in range(1, tp):
        frm = lax.rem(tpi + tp - q, tp)
        remote(ns_v, nr_v.at[frm], n_s.at[q], n_r.at[q], {"tp": partner}).wait_recv()
    norms = nr_v[0]
    for j in range(1, tp):
        norms = norms + nr_v[j]
    gn_ref[...] = norms[0:1, :]
    ln_ref[...] = norms[1:2, :]

    for q in range(1, nz):
        remote(zs_v.at[q], zr_v.at[q], z_s.at[q], z_r.at[q], {"tp": partner}).wait_recv()
        acc = acc + zr_v[q].astype(f32)
    dtok_ref[...] = acc.astype(bf16)

    for cp in sends + relays:
        cp.wait_send()
    for cp in outs:
        cp.wait()


def shards(tokens, routes, gates, cotangent, w_glu, w_lin, w_down):
    ep = lax.axis_size("ep")
    tp = lax.axis_size("tp")
    rows, top = routes.shape
    width = tokens.shape[1]
    units = w_glu.shape[2]
    cap = 3 * rows * top // (2 * ep)
    cap = -(-cap // 16) * 16
    slots = ep * cap
    half = width // CORES
    own = width // tp
    nz = tp // CORES
    vm = pl.BlockSpec(memory_space=pltpu.VMEM)
    hbm = pl.BlockSpec(memory_space=pl.ANY)
    dma = pltpu.SemaphoreType.DMA
    erows = max(8, ep)
    V = pltpu.VMEM
    outs = pl.pallas_call(
        functools.partial(kernel, ep, tp, cap),
        out_shape=(
            jax.ShapeDtypeStruct((rows, own), bf16),
            jax.ShapeDtypeStruct((rows, top), f32),
            jax.ShapeDtypeStruct((width, units), f32),
            jax.ShapeDtypeStruct((width, units), f32),
            jax.ShapeDtypeStruct((units, width), f32),
            jax.ShapeDtypeStruct((1, width), f32),
            jax.ShapeDtypeStruct((1, width), f32),
            jax.ShapeDtypeStruct((1, units), f32),
        ),
        in_specs=[vm] * 7,
        out_specs=(vm, vm, hbm, hbm, hbm, vm, vm, vm),
        scratch_shapes=[
            V((ep, rows, LANES), bf16),
            V((2, ep, cap, half), bf16),
            V((2, CORES, slots, half), bf16),
            V((ep, 8, LANES), f32),
            V((ep, 8, LANES), f32),
            V((3, slots, units), bf16),
            V((3, units, slots), bf16),
            V((nz, slots, own), bf16),
            V((nz, slots, own), bf16),
            V((nz, slots, own), f32),
            V((nz, slots, own), bf16),
            V((nz, slots, own), bf16),
            V((nz, rows, own), bf16),
            V((nz, rows, own), bf16),
            V((tp, erows, LANES), f32),
            V((ep, 8, LANES), f32),
            V((ep, 8, LANES), f32),
            V((2, width), f32),
            V((tp, 2, width), f32),
            V((width, units), f32),
            V((width, units), f32),
            V((units, width), f32),
            dma((2, ep)), dma((2, ep)), dma((ep,)), dma((ep,)), dma((2, ep)), dma((2, ep)),
            dma((nz,)), dma((nz,)), dma((nz, ep)), dma((nz, ep)), dma((nz,)), dma((nz,)),
            dma((tp,)), dma((tp,)), dma((ep,)), dma((ep,)), dma((tp,)), dma((tp,)), dma((3,)),
        ],
        compiler_params=pltpu.CompilerParams(
            collective_id=0, has_side_effects=True, vmem_limit_bytes=40 * 1024 * 1024
        ),
    )(tokens, routes, gates, cotangent, w_glu[0], w_lin[0], w_down[0])
    d_tokens, d_gates, gw, lw, dw, gn, ln, dn = outs
    return (d_tokens, d_gates, gw[None], lw[None], dw[None], gn, ln, dn)


def solution(mesh):
    in_specs = (
        P("ep", None),
        P("ep", None),
        P("ep", None),
        P("ep", None),
        P("ep", None, "tp"),
        P("ep", None, "tp"),
        P("ep", "tp", None),
    )
    out_specs = (
        P("ep", "tp"),
        P("ep", None),
        P("ep", None, "tp"),
        P("ep", None, "tp"),
        P("ep", "tp", None),
        P("ep", None),
        P("ep", None),
        P("ep", "tp"),
    )
    return jax.shard_map(shards, mesh=mesh, in_specs=in_specs, out_specs=out_specs, check_vma=False)
```

```python
import functools

import jax
import jax.numpy as jnp
from jax import lax
from jax.experimental import pallas as pl
from jax.experimental.pallas import tpu as pltpu
from jax.sharding import PartitionSpec as P

clamp_limit = 7.0
sigmoid_scale = 1.702
MESH = pl.DeviceIdType.MESH
LANES = 128
CORES = 2
f32 = jnp.float32
bf16 = jnp.bfloat16


def dot_nn(a, b):
    return lax.dot_general(a, b, (((1,), (0,)), ((), ())), preferred_element_type=f32)


def dot_nt(a, b):
    return lax.dot_general(a, b, (((1,), (1,)), ((), ())), preferred_element_type=f32)


def clamp_backward(glu_pre, lin_pre, back_proj, gate_col):
    glu_clip = jnp.minimum(glu_pre, clamp_limit)
    lin_clip = jnp.clip(lin_pre, -clamp_limit, clamp_limit)
    sig_val = jax.nn.sigmoid(sigmoid_scale * glu_clip)
    glu_act = glu_clip * sig_val
    hidden = glu_act * (lin_clip + 1.0)
    hid_grad = gate_col * back_proj
    act_slope = sig_val + sigmoid_scale * glu_clip * sig_val * (1.0 - sig_val)
    glu_grad = jnp.where(glu_pre < clamp_limit, hid_grad * (lin_clip + 1.0) * act_slope, 0.0)
    lin_grad = jnp.where(jnp.abs(lin_pre) < clamp_limit, hid_grad * glu_act, 0.0)
    return hidden, glu_grad.astype(bf16), lin_grad.astype(bf16)


def kernel(
    ep, tp, cap,
    tok_hbm, routes_hbm, gates_hbm, cot_hbm, wg_hbm, wl_hbm, wd_hbm,
    dtok_ref, dgate_ref, gw_v, lw_v, dw_v, gn_ref, ln_ref, dn_ref,
    tok_ref, routes_ref, gates_ref, cot_ref, wg_ref, wl_ref, wd_ref,
    pt_v, pk_v, snd_v, all_v, gsnd_v, grow_v, bf_v, tr_v,
    ps_v, pr_v, mine_v, xs_v, ret_v, zs_v, zr_v,
    gp_v, gsum_v, gback_v, ns_v, nr_v,
    d_s, d_r, h_s, h_r, g_s, g_r, y_s, y_r, p_s, p_r, x_s, x_r, z_s, z_r,
    a_s, a_r, b_s, b_r, n_s, n_r, l_s,
):
    me = lax.axis_index("ep")
    tpi = lax.axis_index("tp")
    nz = tp // CORES
    core = lax.rem(tpi, CORES)
    chip = lax.div(tpi, CORES)
    other = 1 - core
    partner = chip * CORES + other
    rows = tok_ref.shape[0]
    width = tok_ref.shape[1]
    hidden_units = wg_ref.shape[1]
    half = width // CORES
    own = width // tp
    odd = lax.rem(chip, 2)
    beside = (chip + 1 - 2 * odd) * CORES + core
    loads = []
    for i, (src, dst) in enumerate((
        (routes_hbm, routes_ref), (gates_hbm, gates_ref), (cot_hbm, cot_ref),
        (tok_hbm, tok_ref), (wg_hbm, wg_ref), (wl_hbm, wl_ref), (wd_hbm, wd_ref),
    )):
        cp = pltpu.make_async_copy(src, dst, l_s.at[i])
        cp.start()
        loads.append(cp)

    def ahead(r):
        return lax.rem(me + r, ep)

    def behind(r):
        return lax.rem(me + ep - r, ep)

    barrier = pltpu.get_barrier_semaphore()
    for r in range(1, ep):
        pl.semaphore_signal(barrier, inc=1, device_id={"ep": ahead(r)}, device_id_type=MESH)
    for q in range(1, tp):
        pl.semaphore_signal(
            barrier, inc=1, device_id={"tp": lax.rem(tpi + q, tp)}, device_id_type=MESH
        )

    def remote(src, dst, ss, rs, where):
        return pltpu.make_async_remote_copy(
            src_ref=src, dst_ref=dst, send_sem=ss, recv_sem=rs,
            device_id=where, device_id_type=MESH,
        )

    loads[0].wait()
    loads[1].wait()
    rel = routes_ref[...] - me
    rel = jnp.where(rel < 0, rel + ep, rel)
    erows = gp_v.shape[1]
    sub = lax.broadcasted_iota(jnp.int32, (erows, rows), 0)
    first, second = sub == rel[0:1, :], sub == rel[1:2, :]
    mask = jnp.where(first, 1.0, 0.0) + jnp.where(second, 1.0, 0.0)
    gate_of = jnp.where(first, gates_ref[0:1, :], 0.0) + jnp.where(second, gates_ref[1:2, :], 0.0)
    before = lax.broadcasted_iota(jnp.int32, (rows, rows), 0) < lax.broadcasted_iota(
        jnp.int32, (rows, rows), 1
    )
    rank = dot_nn(mask.astype(bf16), jnp.where(before, 1.0, 0.0).astype(bf16))
    place = jnp.where(mask > 0.5, rank, -1.0)
    slot_at = lax.broadcasted_iota(jnp.int32, (LANES, rows), 0).astype(f32)
    hits = [jnp.where(slot_at == place[r:r + 1, :], 1.0, 0.0) for r in range(ep)]
    picks = [hit[:cap, :].astype(bf16) for hit in hits]
    square = lax.broadcasted_iota(jnp.int32, (LANES, LANES), 0) == lax.broadcasted_iota(
        jnp.int32, (LANES, LANES), 1
    )
    sends = []

    narrow = half // 8
    pieces = (
        (1, 0, half // 2, True),
        (0, 0, narrow, True),
        (0, 2 * narrow, half - 2 * narrow, False),
    )
    swapped = [i for i, piece in enumerate(pieces) if piece[3]]
    refs = (tok_ref, cot_ref)

    def window(i, whose):
        a, off, w, shared = pieces[i]
        if shared:
            off = off + whose * w
        return a, (pl.ds(pl.multiple_of(off, LANES), w) if shared else pl.ds(off, w))

    def area(buf, i, r, whose, which):
        a, cols = window(i, whose)
        return buf.at[a, which, pl.ds(r * cap, cap), cols]

    def dispatch(i, r):
        a, cols = window(i, odd)
        return remote(
            snd_v.at[a, r, :, cols], area(all_v, i, r, odd, core),
            d_s.at[i, r], d_r.at[i, r], {"ep": ahead(r)},
        )

    def swap(i, r, whose):
        at = area(all_v, i, r, whose, core)
        return remote(at, at, h_s.at[i, r], h_r.at[i, r], {"tp": beside})

    def relay(k, i, r, whose, which):
        at = area(all_v, i, r, whose, which)
        return remote(at, at, y_s.at[k, r], y_r.at[k, r], {"tp": partner})

    loads[2].wait()
    loads[3].wait()
    waited = False
    for i in range(len(pieces)):
        a, off, w, shared = pieces[i]
        start = core * half + off + (odd * w if shared else 0)
        src_cols = pl.ds(pl.multiple_of(start, LANES), w)
        for r in range(1, ep):
            snd_v[a, r, :, window(i, odd)[1]] = dot_nn(
                picks[r], refs[a][:, src_cols]
            ).astype(bf16)
            if not waited:
                pl.semaphore_wait(barrier, ep - 1 + tp - 1)
                waited = True
            cp = dispatch(i, r)
            cp.start()
            sends.append(cp)
    for r in range(ep):
        col = jnp.sum(hits[r] * gate_of[r:r + 1, :], axis=1, keepdims=True)
        row = jnp.sum(jnp.where(square, col, 0.0), axis=0, keepdims=True)
        if r == 0:
            grow_v[0] = jnp.broadcast_to(row, (8, LANES))
        else:
            gsnd_v[r] = jnp.broadcast_to(row, (8, LANES))
            cp = remote(gsnd_v.at[r], grow_v.at[r], g_s.at[r], g_r.at[r], {"ep": ahead(r)})
            cp.start()
            sends.append(cp)
    for a, ref in ((0, tok_ref), (1, cot_ref)):
        for h in range(CORES):
            all_v[a, h, 0:cap, :] = dot_nn(picks[0], ref[:, h * half:(h + 1) * half]).astype(bf16)
    for r in range(ep):
        pk_v[r] = hits[r].astype(bf16)
        pt_v[r] = hits[r].T.astype(bf16)

    eye = lax.broadcasted_iota(jnp.int32, (cap, LANES), 0) == lax.broadcasted_iota(
        jnp.int32, (cap, LANES), 1
    )

    gp_v[tpi] = jnp.zeros(gp_v.shape[1:], f32)

    def forward(r):
        rs = slice(r * cap, (r + 1) * cap)
        glu_pre = jnp.zeros((cap, hidden_units), f32)
        lin_pre = glu_pre
        back = glu_pre
        for h in range(CORES):
            hs = slice(h * half, (h + 1) * half)
            glu_pre = glu_pre + dot_nn(all_v[0, h, rs, :], wg_ref[hs, :])
            lin_pre = lin_pre + dot_nn(all_v[0, h, rs, :], wl_ref[hs, :])
            back = back + dot_nt(all_v[1, h, rs, :], wd_ref[:, hs])
        gate_col = jnp.sum(jnp.where(eye, grow_v[r, 0:1, :], 0.0), axis=1, keepdims=True)
        hidden, glu_bf, lin_bf = clamp_backward(glu_pre, lin_pre, back, gate_col)
        part = jnp.sum(back * hidden, axis=1, keepdims=True)
        gp_v[tpi, r:r + 1, :] = jnp.sum(jnp.where(eye, part, 0.0), axis=0, keepdims=True)
        bf_v[0, rs, :] = glu_bf
        bf_v[1, rs, :] = lin_bf
        bf_v[2, rs, :] = (gate_col * hidden).astype(bf16)

    count = len(pieces)
    for i in swapped:
        for r in range(1, ep):
            dispatch(i, r).wait_recv()
            for cp in (swap(i, r, odd), relay(i, i, r, odd, core)):
                cp.start()
                sends.append(cp)
    for cp in loads[4:]:
        cp.wait()
    forward(0)
    for r in range(1, ep):
        for n, i in enumerate(swapped):
            swap(i, r, 1 - odd).wait_recv()
            cp = relay(count + n, i, r, 1 - odd, core)
            cp.start()
            sends.append(cp)
        for i in range(count):
            if i not in swapped:
                dispatch(i, r).wait_recv()
                cp = relay(i, i, r, odd, core)
                cp.start()
                sends.append(cp)
    for r in range(1, ep):
        for i in range(count):
            relay(i, i, r, odd, other).wait_recv()
        for n, i in enumerate(swapped):
            relay(count + n, i, r, 1 - odd, other).wait_recv()
        remote(gsnd_v.at[r], grow_v.at[r], g_s.at[r], g_r.at[r], {"ep": ahead(r)}).wait_recv()
        forward(r)

    for q in range(1, tp):
        cp = remote(gp_v.at[tpi], gp_v.at[tpi], a_s.at[q], a_r.at[q], {"tp": lax.rem(tpi + q, tp)})
        cp.start()
        sends.append(cp)

    def input_cols(q, which):
        z = lax.rem(chip + q, nz)
        at = pl.ds(pl.multiple_of((z * CORES + which) * own, own), own)
        return dot_nt(bf_v[0], wg_ref[at, :]) + dot_nt(bf_v[1], wl_ref[at, :])

    order = list(range(1, nz)) + [0]
    for q in order:
        ps_v[q] = input_cols(q, other).astype(bf16)
        cp = remote(ps_v.at[q], pr_v.at[q], p_s.at[q], p_r.at[q], {"tp": partner})
        cp.start()
        sends.append(cp)
    for q in order:
        mine_v[q] = input_cols(q, core)
    for q in order:
        remote(ps_v.at[q], pr_v.at[q], p_s.at[q], p_r.at[q], {"tp": partner}).wait_recv()
        total = (mine_v[q] + pr_v[q].astype(f32)).astype(bf16)
        ret_v[q, 0:cap, :] = total[0:cap, :]
        for r in range(1, ep):
            rs = slice(r * cap, (r + 1) * cap)
            xs_v[q, rs, :] = total[rs, :]
        for r in range(1, ep):
            rs = pl.ds(r * cap, cap)
            cp = remote(
                xs_v.at[q, rs, :], ret_v.at[q, rs, :],
                x_s.at[q, r], x_r.at[q, r], {"ep": behind(r)},
            )
            cp.start()
            sends.append(cp)

    for i in range(3):
        tr_v[i] = bf_v[i].astype(f32).T.astype(bf16)
    step = min(512, half)
    for h in range(CORES):
        for c0 in range(0, half, step):
            cols = slice(h * half + c0, h * half + c0 + step)
            x = all_v[0, h, :, c0:c0 + step]
            for i, (w_v, at) in enumerate(((gw_v, 0), (lw_v, 1))):
                w = dot_nn(tr_v[i], x)
                ns_v[at:at + 1, cols] = jnp.sum(w * w, axis=0, keepdims=True)
                w_v[cols, :] = w.T
    nr_v[tpi] = ns_v[...]
    for q in range(1, tp):
        cp = remote(ns_v, nr_v.at[tpi], n_s.at[q], n_r.at[q], {"tp": lax.rem(tpi + q, tp)})
        cp.start()
        sends.append(cp)

    for q in range(1, tp):
        frm = lax.rem(tpi + tp - q, tp)
        remote(gp_v.at[tpi], gp_v.at[frm], a_s.at[q], a_r.at[q], {"tp": partner}).wait_recv()
    gsum = gp_v[0]
    for j in range(1, tp):
        gsum = gsum + gp_v[j]
    gback_v[0, 0:1, :] = gsum[0:1, :]
    for r in range(1, ep):
        gsum_v[r] = jnp.broadcast_to(gsum[r:r + 1, :], (8, LANES))
        cp = remote(gsum_v.at[r], gback_v.at[r], b_s.at[r], b_r.at[r], {"ep": behind(r)})
        cp.start()
        sends.append(cp)

    norm = jnp.zeros((hidden_units, 1), f32)
    for h in range(CORES):
        for c0 in range(0, half, step):
            cols = slice(h * half + c0, h * half + c0 + step)
            w = dot_nn(tr_v[2], all_v[1, h, :, c0:c0 + step])
            norm = norm + jnp.sum(w * w, axis=1, keepdims=True)
            dw_v[:, cols] = w
    diag = lax.broadcasted_iota(jnp.int32, (hidden_units, hidden_units), 0) == (
        lax.broadcasted_iota(jnp.int32, (hidden_units, hidden_units), 1)
    )
    dn_ref[...] = jnp.sum(jnp.where(diag, norm, 0.0), axis=0, keepdims=True)

    acc = None
    for q in order:
        part = None
        for r in range(ep):
            rs = pl.ds(r * cap, cap)
            if r > 0:
                remote(
                    xs_v.at[q, rs, :], ret_v.at[q, rs, :],
                    x_s.at[q, r], x_r.at[q, r], {"ep": behind(r)},
                ).wait_recv()
            term = dot_nn(pt_v[r][:, :cap], ret_v[q, r * cap:(r + 1) * cap, :])
            part = term if part is None else part + term
        if q == 0:
            acc = part
        else:
            zs_v[q] = part.astype(bf16)
            to = lax.rem(chip + q, nz) * CORES + core
            cp = remote(zs_v.at[q], zr_v.at[q], z_s.at[q], z_r.at[q], {"tp": to})
            cp.start()
            sends.append(cp)

    res = [jnp.zeros((1, rows), f32), jnp.zeros((1, rows), f32)]
    for r in range(ep):
        if r > 0:
            remote(
                gsum_v.at[r], gback_v.at[r], b_s.at[r], b_r.at[r], {"ep": behind(r)}
            ).wait_recv()
        col = jnp.sum(jnp.where(square, gback_v[r, 0:1, :], 0.0), axis=1, keepdims=True)
        val = jnp.sum(pk_v[r].astype(f32) * col, axis=0, keepdims=True)
        for k in range(2):
            res[k] = res[k] + jnp.where(rel[k:k + 1, :] == r, val, 0.0)
    dgate_ref[0:1, :] = res[0]
    dgate_ref[1:2, :] = res[1]

    for q in range(1, tp):
        frm = lax.rem(tpi + tp - q, tp)
        remote(ns_v, nr_v.at[frm], n_s.at[q], n_r.at[q], {"tp": partner}).wait_recv()
    norms = nr_v[0]
    for j in range(1, tp):
        norms = norms + nr_v[j]
    gn_ref[...] = norms[0:1, :]
    ln_ref[...] = norms[1:2, :]

    for q in range(1, nz):
        remote(zs_v.at[q], zr_v.at[q], z_s.at[q], z_r.at[q], {"tp": partner}).wait_recv()
        acc = acc + zr_v[q].astype(f32)
    dtok_ref[...] = acc.astype(bf16)

    for cp in sends:
        cp.wait_send()


def write_out(*refs):
    count = (len(refs) - 1) // 2
    copies = [
        pltpu.make_async_copy(refs[i], refs[count + i], refs[-1].at[i]) for i in range(count)
    ]
    for cp in copies:
        cp.start()
    for cp in copies:
        cp.wait()


def shards(tokens, routes, gates, cotangent, w_glu, w_lin, w_down):
    ep = lax.axis_size("ep")
    tp = lax.axis_size("tp")
    rows, top = routes.shape
    width = tokens.shape[1]
    units = w_glu.shape[2]
    cap = 3 * rows * top // (2 * ep)
    cap = -(-cap // 16) * 16
    slots = ep * cap
    half = width // CORES
    own = width // tp
    nz = tp // CORES
    vm = pl.BlockSpec(memory_space=pltpu.VMEM)
    hbm = pl.BlockSpec(memory_space=pltpu.HBM)
    dma = pltpu.SemaphoreType.DMA
    erows = max(8, ep)
    V = pltpu.VMEM
    out_shape = (
        jax.ShapeDtypeStruct((rows, own), bf16),
        jax.ShapeDtypeStruct((top, rows), f32),
        jax.ShapeDtypeStruct((width, units), f32),
        jax.ShapeDtypeStruct((width, units), f32),
        jax.ShapeDtypeStruct((units, width), f32),
        jax.ShapeDtypeStruct((1, width), f32),
        jax.ShapeDtypeStruct((1, width), f32),
        jax.ShapeDtypeStruct((1, units), f32),
    )
    outs = pl.pallas_call(
        functools.partial(kernel, ep, tp, cap),
        out_shape=out_shape,
        in_specs=[hbm] * 7,
        out_specs=(vm,) * 8,
        scratch_shapes=[
            V((rows, width), bf16),
            V((top, rows), jnp.int32),
            V((top, rows), f32),
            V((rows, width), bf16),
            V((width, units), bf16),
            V((width, units), bf16),
            V((units, width), bf16),
            V((ep, rows, LANES), bf16),
            V((ep, rows, LANES), bf16),
            V((2, ep, cap, half), bf16),
            V((2, CORES, slots, half), bf16),
            V((ep, 8, LANES), f32),
            V((ep, 8, LANES), f32),
            V((3, slots, units), bf16),
            V((3, units, slots), bf16),
            V((nz, slots, own), bf16),
            V((nz, slots, own), bf16),
            V((nz, slots, own), f32),
            V((nz, slots, own), bf16),
            V((nz, slots, own), bf16),
            V((nz, rows, own), bf16),
            V((nz, rows, own), bf16),
            V((tp, erows, LANES), f32),
            V((ep, 8, LANES), f32),
            V((ep, 8, LANES), f32),
            V((2, width), f32),
            V((tp, 2, width), f32),
            dma((3, ep)), dma((3, ep)), dma((2, ep)), dma((2, ep)), dma((ep,)), dma((ep,)),
            dma((5, ep)), dma((5, ep)),
            dma((nz,)), dma((nz,)), dma((nz, ep)), dma((nz, ep)), dma((nz,)), dma((nz,)),
            dma((tp,)), dma((tp,)), dma((ep,)), dma((ep,)), dma((tp,)), dma((tp,)), dma((7,)),
        ],
        compiler_params=pltpu.CompilerParams(
            collective_id=0, has_side_effects=True, vmem_limit_bytes=28 * 1024 * 1024
        ),
    )(*(pltpu.with_memory_space_constraint(x, pltpu.HBM) for x in (
        tokens, routes.T, gates.T, cotangent, w_glu[0], w_lin[0], w_down[0]
    )))
    outs = pl.pallas_call(
        write_out,
        out_shape=out_shape,
        in_specs=[vm] * len(out_shape),
        out_specs=(hbm,) * len(out_shape),
        scratch_shapes=[dma((len(out_shape),))],
        compiler_params=pltpu.CompilerParams(vmem_limit_bytes=28 * 1024 * 1024),
    )(*outs)
    d_tokens, d_gates, gw, lw, dw, gn, ln, dn = outs
    return (d_tokens, d_gates.T, gw[None], lw[None], dw[None], gn, ln, dn)


def solution(mesh):
    in_specs = (
        P("ep", None),
        P("ep", None),
        P("ep", None),
        P("ep", None),
        P("ep", None, "tp"),
        P("ep", None, "tp"),
        P("ep", "tp", None),
    )
    out_specs = (
        P("ep", "tp"),
        P("ep", None),
        P("ep", None, "tp"),
        P("ep", None, "tp"),
        P("ep", "tp", None),
        P("ep", None),
        P("ep", None),
        P("ep", "tp"),
    )
    return jax.shard_map(shards, mesh=mesh, in_specs=in_specs, out_specs=out_specs, check_vma=False)
```

```python
import functools

import jax
import jax.numpy as jnp
from jax import lax
from jax.experimental import pallas as pl
from jax.experimental.pallas import tpu as pltpu
from jax.sharding import PartitionSpec as P

clamp_limit = 7.0
sigmoid_scale = 1.702
MESH = pl.DeviceIdType.MESH
LANES = 128
CORES = 2
f32 = jnp.float32
bf16 = jnp.bfloat16


def dot_nn(a, b):
    return lax.dot_general(a, b, (((1,), (0,)), ((), ())), preferred_element_type=f32)


def dot_nt(a, b):
    return lax.dot_general(a, b, (((1,), (1,)), ((), ())), preferred_element_type=f32)


def clamp_backward(glu_pre, lin_pre, back_proj, gate_col):
    glu_clip = jnp.minimum(glu_pre, clamp_limit)
    lin_clip = jnp.clip(lin_pre, -clamp_limit, clamp_limit)
    sig_val = jax.nn.sigmoid(sigmoid_scale * glu_clip)
    glu_act = glu_clip * sig_val
    hidden = glu_act * (lin_clip + 1.0)
    hid_grad = gate_col * back_proj
    act_slope = sig_val + sigmoid_scale * glu_clip * sig_val * (1.0 - sig_val)
    glu_grad = jnp.where(glu_pre < clamp_limit, hid_grad * (lin_clip + 1.0) * act_slope, 0.0)
    lin_grad = jnp.where(jnp.abs(lin_pre) < clamp_limit, hid_grad * glu_act, 0.0)
    return hidden, glu_grad.astype(bf16), lin_grad.astype(bf16)


def kernel(
    ep, tp, cap,
    tok_hbm, routes_hbm, gates_hbm, cot_hbm, wg_hbm, wl_hbm, wd_hbm,
    dtok_ref, dgate_ref, gw_v, lw_v, dw_v, gn_ref, ln_ref, dn_ref,
    tok_ref, routes_ref, gates_ref, cot_ref, wg_ref, wl_ref, wd_ref,
    pt_v, pk_v, snd_v, all_v, gsnd_v, grow_v, bf_v, tr_v,
    ps_v, pr_v, mine_v, xs_v, ret_v, zs_v, zr_v,
    gp_v, gsum_v, gback_v, ns_v, nr_v,
    d_s, d_r, h_s, h_r, g_s, g_r, y_s, y_r, p_s, p_r, x_s, x_r, z_s, z_r,
    a_s, a_r, b_s, b_r, n_s, n_r, l_s,
):
    me = lax.axis_index("ep")
    tpi = lax.axis_index("tp")
    nz = tp // CORES
    core = lax.rem(tpi, CORES)
    chip = lax.div(tpi, CORES)
    other = 1 - core
    partner = chip * CORES + other
    rows = tok_ref.shape[0]
    width = tok_ref.shape[1]
    hidden_units = wg_ref.shape[1]
    half = width // CORES
    own = width // tp
    odd = lax.rem(chip, 2)
    beside = (chip + 1 - 2 * odd) * CORES + core
    loads = []
    for i, (src, dst) in enumerate((
        (routes_hbm, routes_ref), (gates_hbm, gates_ref), (cot_hbm, cot_ref),
        (tok_hbm, tok_ref), (wg_hbm, wg_ref), (wl_hbm, wl_ref), (wd_hbm, wd_ref),
    )):
        cp = pltpu.make_async_copy(src, dst, l_s.at[i])
        cp.start()
        loads.append(cp)

    def ahead(r):
        return lax.rem(me + r, ep)

    def behind(r):
        return lax.rem(me + ep - r, ep)

    barrier = pltpu.get_barrier_semaphore()
    for r in range(1, ep):
        pl.semaphore_signal(barrier, inc=1, device_id={"ep": ahead(r)}, device_id_type=MESH)
    for q in range(1, tp):
        pl.semaphore_signal(
            barrier, inc=1, device_id={"tp": lax.rem(tpi + q, tp)}, device_id_type=MESH
        )

    def remote(src, dst, ss, rs, where):
        return pltpu.make_async_remote_copy(
            src_ref=src, dst_ref=dst, send_sem=ss, recv_sem=rs,
            device_id=where, device_id_type=MESH,
        )

    loads[0].wait()
    loads[1].wait()
    rel = routes_ref[...] - me
    rel = jnp.where(rel < 0, rel + ep, rel)
    erows = gp_v.shape[1]
    sub = lax.broadcasted_iota(jnp.int32, (erows, rows), 0)
    first, second = sub == rel[0:1, :], sub == rel[1:2, :]
    mask = jnp.where(first, 1.0, 0.0) + jnp.where(second, 1.0, 0.0)
    gate_of = jnp.where(first, gates_ref[0:1, :], 0.0) + jnp.where(second, gates_ref[1:2, :], 0.0)
    before = lax.broadcasted_iota(jnp.int32, (rows, rows), 0) < lax.broadcasted_iota(
        jnp.int32, (rows, rows), 1
    )
    rank = dot_nn(mask.astype(bf16), jnp.where(before, 1.0, 0.0).astype(bf16))
    place = jnp.where(mask > 0.5, rank, -1.0)
    slot_at = lax.broadcasted_iota(jnp.int32, (LANES, rows), 0).astype(f32)
    hits = [jnp.where(slot_at == place[r:r + 1, :], 1.0, 0.0) for r in range(ep)]
    picks = [hit[:cap, :].astype(bf16) for hit in hits]
    square = lax.broadcasted_iota(jnp.int32, (LANES, LANES), 0) == lax.broadcasted_iota(
        jnp.int32, (LANES, LANES), 1
    )
    sends = []

    narrow = half // 8
    pieces = (
        (1, 0, half // 2, True),
        (0, 0, narrow, True),
        (0, 2 * narrow, half - 2 * narrow, False),
    )
    swapped = [i for i, piece in enumerate(pieces) if piece[3]]
    refs = (tok_ref, cot_ref)

    def window(i, whose):
        a, off, w, shared = pieces[i]
        if shared:
            off = off + whose * w
        return a, (pl.ds(pl.multiple_of(off, LANES), w) if shared else pl.ds(off, w))

    def area(buf, i, r, whose, which):
        a, cols = window(i, whose)
        return buf.at[a, which, pl.ds(r * cap, cap), cols]

    def dispatch(i, r):
        a, cols = window(i, odd)
        return remote(
            snd_v.at[a, r, :, cols], area(all_v, i, r, odd, core),
            d_s.at[i, r], d_r.at[i, r], {"ep": ahead(r)},
        )

    def swap(i, r, whose):
        at = area(all_v, i, r, whose, core)
        return remote(at, at, h_s.at[i, r], h_r.at[i, r], {"tp": beside})

    def relay(k, i, r, whose, which):
        at = area(all_v, i, r, whose, which)
        return remote(at, at, y_s.at[k, r], y_r.at[k, r], {"tp": partner})

    loads[2].wait()
    loads[3].wait()
    waited = False
    for i in range(len(pieces)):
        a, off, w, shared = pieces[i]
        start = core * half + off + (odd * w if shared else 0)
        src_cols = pl.ds(pl.multiple_of(start, LANES), w)
        for r in range(1, ep):
            snd_v[a, r, :, window(i, odd)[1]] = dot_nn(
                picks[r], refs[a][:, src_cols]
            ).astype(bf16)
            if not waited:
                pl.semaphore_wait(barrier, ep - 1 + tp - 1)
                waited = True
            cp = dispatch(i, r)
            cp.start()
            sends.append(cp)
    for r in range(ep):
        col = jnp.sum(hits[r] * gate_of[r:r + 1, :], axis=1, keepdims=True)
        row = jnp.sum(jnp.where(square, col, 0.0), axis=0, keepdims=True)
        if r == 0:
            grow_v[0] = jnp.broadcast_to(row, (8, LANES))
        else:
            gsnd_v[r] = jnp.broadcast_to(row, (8, LANES))
            cp = remote(gsnd_v.at[r], grow_v.at[r], g_s.at[r], g_r.at[r], {"ep": ahead(r)})
            cp.start()
            sends.append(cp)
    for a, ref in ((0, tok_ref), (1, cot_ref)):
        for h in range(CORES):
            all_v[a, h, 0:cap, :] = dot_nn(picks[0], ref[:, h * half:(h + 1) * half]).astype(bf16)
    for r in range(ep):
        pk_v[r] = hits[r].astype(bf16)
        pt_v[r] = hits[r].T.astype(bf16)

    eye = lax.broadcasted_iota(jnp.int32, (cap, LANES), 0) == lax.broadcasted_iota(
        jnp.int32, (cap, LANES), 1
    )

    gp_v[tpi] = jnp.zeros(gp_v.shape[1:], f32)

    def forward(r):
        rs = slice(r * cap, (r + 1) * cap)
        glu_pre = jnp.zeros((cap, hidden_units), f32)
        lin_pre = glu_pre
        back = glu_pre
        for h in range(CORES):
            hs = slice(h * half, (h + 1) * half)
            glu_pre = glu_pre + dot_nn(all_v[0, h, rs, :], wg_ref[hs, :])
            lin_pre = lin_pre + dot_nn(all_v[0, h, rs, :], wl_ref[hs, :])
            back = back + dot_nt(all_v[1, h, rs, :], wd_ref[:, hs])
        gate_col = jnp.sum(jnp.where(eye, grow_v[r, 0:1, :], 0.0), axis=1, keepdims=True)
        hidden, glu_bf, lin_bf = clamp_backward(glu_pre, lin_pre, back, gate_col)
        part = jnp.sum(back * hidden, axis=1, keepdims=True)
        gp_v[tpi, r:r + 1, :] = jnp.sum(jnp.where(eye, part, 0.0), axis=0, keepdims=True)
        bf_v[0, rs, :] = glu_bf
        bf_v[1, rs, :] = lin_bf
        bf_v[2, rs, :] = (gate_col * hidden).astype(bf16)

    count = len(pieces)
    for i in swapped:
        for r in range(1, ep):
            dispatch(i, r).wait_recv()
            for cp in (swap(i, r, odd), relay(i, i, r, odd, core)):
                cp.start()
                sends.append(cp)
    for cp in loads[4:]:
        cp.wait()
    order = list(range(1, nz)) + [0]

    def input_cols(q, which, rs):
        z = lax.rem(chip + q, nz)
        at = pl.ds(pl.multiple_of((z * CORES + which) * own, own), own)
        return dot_nt(bf_v[0, rs, :], wg_ref[at, :]) + dot_nt(bf_v[1, rs, :], wl_ref[at, :])

    def to_partner(r):
        at = pl.ds(r * cap, cap)
        return remote(ps_v.at[:, at, :], pr_v.at[:, at, :], p_s.at[r], p_r.at[r], {"tp": partner})

    def block(r):
        if r > 0:
            for i in range(count):
                relay(i, i, r, odd, other).wait_recv()
            for n, i in enumerate(swapped):
                relay(count + n, i, r, 1 - odd, other).wait_recv()
            remote(gsnd_v.at[r], grow_v.at[r], g_s.at[r], g_r.at[r], {"ep": ahead(r)}).wait_recv()
        forward(r)
        rs = slice(r * cap, (r + 1) * cap)
        for q in order:
            ps_v[q, rs, :] = input_cols(q, other, rs).astype(bf16)
        cp = to_partner(r)
        cp.start()
        sends.append(cp)
        for q in order:
            mine_v[q, rs, :] = input_cols(q, core, rs)

    def arrive(r):
        for n, i in enumerate(swapped):
            swap(i, r, 1 - odd).wait_recv()
            cp = relay(count + n, i, r, 1 - odd, core)
            cp.start()
            sends.append(cp)
        for i in range(count):
            if i not in swapped:
                dispatch(i, r).wait_recv()
                cp = relay(i, i, r, odd, core)
                cp.start()
                sends.append(cp)

    middle = ep // 2
    turn = [middle] + [r for r in range(1, ep) if r != middle]
    block(0)
    for n, r in enumerate(turn):
        arrive(r)
        if n > 0:
            block(turn[n - 1])
    block(turn[-1])

    for r in range(ep):
        to_partner(r).wait_recv()
    for q in order:
        total = (mine_v[q] + pr_v[q].astype(f32)).astype(bf16)
        ret_v[q, 0:cap, :] = total[0:cap, :]
        for r in range(1, ep):
            rs = slice(r * cap, (r + 1) * cap)
            xs_v[q, rs, :] = total[rs, :]
        for r in range(1, ep):
            rs = pl.ds(r * cap, cap)
            cp = remote(
                xs_v.at[q, rs, :], ret_v.at[q, rs, :],
                x_s.at[q, r], x_r.at[q, r], {"ep": behind(r)},
            )
            cp.start()
            sends.append(cp)

    for q in range(1, tp):
        cp = remote(gp_v.at[tpi], gp_v.at[tpi], a_s.at[q], a_r.at[q], {"tp": lax.rem(tpi + q, tp)})
        cp.start()
        sends.append(cp)

    for i in range(3):
        tr_v[i] = bf_v[i].astype(f32).T.astype(bf16)
    step = min(512, half)
    for h in range(CORES):
        for c0 in range(0, half, step):
            cols = slice(h * half + c0, h * half + c0 + step)
            x = all_v[0, h, :, c0:c0 + step]
            for i, (w_v, at) in enumerate(((gw_v, 0), (lw_v, 1))):
                w = dot_nn(tr_v[i], x)
                ns_v[at:at + 1, cols] = jnp.sum(w * w, axis=0, keepdims=True)
                w_v[cols, :] = w.T
    nr_v[tpi] = ns_v[...]
    for q in range(1, tp):
        cp = remote(ns_v, nr_v.at[tpi], n_s.at[q], n_r.at[q], {"tp": lax.rem(tpi + q, tp)})
        cp.start()
        sends.append(cp)

    for q in range(1, tp):
        frm = lax.rem(tpi + tp - q, tp)
        remote(gp_v.at[tpi], gp_v.at[frm], a_s.at[q], a_r.at[q], {"tp": partner}).wait_recv()
    gsum = gp_v[0]
    for j in range(1, tp):
        gsum = gsum + gp_v[j]
    gback_v[0, 0:1, :] = gsum[0:1, :]
    for r in range(1, ep):
        gsum_v[r] = jnp.broadcast_to(gsum[r:r + 1, :], (8, LANES))
        cp = remote(gsum_v.at[r], gback_v.at[r], b_s.at[r], b_r.at[r], {"ep": behind(r)})
        cp.start()
        sends.append(cp)

    norm = jnp.zeros((hidden_units, 1), f32)
    for h in range(CORES):
        for c0 in range(0, half, step):
            cols = slice(h * half + c0, h * half + c0 + step)
            w = dot_nn(tr_v[2], all_v[1, h, :, c0:c0 + step])
            norm = norm + jnp.sum(w * w, axis=1, keepdims=True)
            dw_v[:, cols] = w
    diag = lax.broadcasted_iota(jnp.int32, (hidden_units, hidden_units), 0) == (
        lax.broadcasted_iota(jnp.int32, (hidden_units, hidden_units), 1)
    )
    dn_ref[...] = jnp.sum(jnp.where(diag, norm, 0.0), axis=0, keepdims=True)

    acc = None
    for q in order:
        part = None
        for r in range(ep):
            rs = pl.ds(r * cap, cap)
            if r > 0:
                remote(
                    xs_v.at[q, rs, :], ret_v.at[q, rs, :],
                    x_s.at[q, r], x_r.at[q, r], {"ep": behind(r)},
                ).wait_recv()
            term = dot_nn(pt_v[r][:, :cap], ret_v[q, r * cap:(r + 1) * cap, :])
            part = term if part is None else part + term
        if q == 0:
            acc = part
        else:
            zs_v[q] = part.astype(bf16)
            to = lax.rem(chip + q, nz) * CORES + core
            cp = remote(zs_v.at[q], zr_v.at[q], z_s.at[q], z_r.at[q], {"tp": to})
            cp.start()
            sends.append(cp)

    res = [jnp.zeros((1, rows), f32), jnp.zeros((1, rows), f32)]
    for r in range(ep):
        if r > 0:
            remote(
                gsum_v.at[r], gback_v.at[r], b_s.at[r], b_r.at[r], {"ep": behind(r)}
            ).wait_recv()
        col = jnp.sum(jnp.where(square, gback_v[r, 0:1, :], 0.0), axis=1, keepdims=True)
        val = jnp.sum(pk_v[r].astype(f32) * col, axis=0, keepdims=True)
        for k in range(2):
            res[k] = res[k] + jnp.where(rel[k:k + 1, :] == r, val, 0.0)
    dgate_ref[0:1, :] = res[0]
    dgate_ref[1:2, :] = res[1]

    for q in range(1, tp):
        frm = lax.rem(tpi + tp - q, tp)
        remote(ns_v, nr_v.at[frm], n_s.at[q], n_r.at[q], {"tp": partner}).wait_recv()
    norms = nr_v[0]
    for j in range(1, tp):
        norms = norms + nr_v[j]
    gn_ref[...] = norms[0:1, :]
    ln_ref[...] = norms[1:2, :]

    for q in range(1, nz):
        remote(zs_v.at[q], zr_v.at[q], z_s.at[q], z_r.at[q], {"tp": partner}).wait_recv()
        acc = acc + zr_v[q].astype(f32)
    dtok_ref[...] = acc.astype(bf16)

    for cp in sends:
        cp.wait_send()


def write_out(*refs):
    count = (len(refs) - 1) // 2
    copies = [
        pltpu.make_async_copy(refs[i], refs[count + i], refs[-1].at[i]) for i in range(count)
    ]
    for cp in copies:
        cp.start()
    for cp in copies:
        cp.wait()


def shards(tokens, routes, gates, cotangent, w_glu, w_lin, w_down):
    ep = lax.axis_size("ep")
    tp = lax.axis_size("tp")
    rows, top = routes.shape
    width = tokens.shape[1]
    units = w_glu.shape[2]
    cap = 3 * rows * top // (2 * ep)
    cap = -(-cap // 16) * 16
    slots = ep * cap
    half = width // CORES
    own = width // tp
    nz = tp // CORES
    vm = pl.BlockSpec(memory_space=pltpu.VMEM)
    hbm = pl.BlockSpec(memory_space=pltpu.HBM)
    dma = pltpu.SemaphoreType.DMA
    erows = max(8, ep)
    V = pltpu.VMEM
    out_shape = (
        jax.ShapeDtypeStruct((rows, own), bf16),
        jax.ShapeDtypeStruct((top, rows), f32),
        jax.ShapeDtypeStruct((width, units), f32),
        jax.ShapeDtypeStruct((width, units), f32),
        jax.ShapeDtypeStruct((units, width), f32),
        jax.ShapeDtypeStruct((1, width), f32),
        jax.ShapeDtypeStruct((1, width), f32),
        jax.ShapeDtypeStruct((1, units), f32),
    )
    outs = pl.pallas_call(
        functools.partial(kernel, ep, tp, cap),
        out_shape=out_shape,
        in_specs=[hbm] * 7,
        out_specs=(vm,) * 8,
        scratch_shapes=[
            V((rows, width), bf16),
            V((top, rows), jnp.int32),
            V((top, rows), f32),
            V((rows, width), bf16),
            V((width, units), bf16),
            V((width, units), bf16),
            V((units, width), bf16),
            V((ep, rows, LANES), bf16),
            V((ep, rows, LANES), bf16),
            V((2, ep, cap, half), bf16),
            V((2, CORES, slots, half), bf16),
            V((ep, 8, LANES), f32),
            V((ep, 8, LANES), f32),
            V((3, slots, units), bf16),
            V((3, units, slots), bf16),
            V((nz, slots, own), bf16),
            V((nz, slots, own), bf16),
            V((nz, slots, own), f32),
            V((nz, slots, own), bf16),
            V((nz, slots, own), bf16),
            V((nz, rows, own), bf16),
            V((nz, rows, own), bf16),
            V((tp, erows, LANES), f32),
            V((ep, 8, LANES), f32),
            V((ep, 8, LANES), f32),
            V((2, width), f32),
            V((tp, 2, width), f32),
            dma((3, ep)), dma((3, ep)), dma((2, ep)), dma((2, ep)), dma((ep,)), dma((ep,)),
            dma((5, ep)), dma((5, ep)),
            dma((ep,)), dma((ep,)), dma((nz, ep)), dma((nz, ep)), dma((nz,)), dma((nz,)),
            dma((tp,)), dma((tp,)), dma((ep,)), dma((ep,)), dma((tp,)), dma((tp,)), dma((7,)),
        ],
        compiler_params=pltpu.CompilerParams(
            collective_id=0, has_side_effects=True, vmem_limit_bytes=28 * 1024 * 1024
        ),
    )(*(pltpu.with_memory_space_constraint(x, pltpu.HBM) for x in (
        tokens, routes.T, gates.T, cotangent, w_glu[0], w_lin[0], w_down[0]
    )))
    outs = pl.pallas_call(
        write_out,
        out_shape=out_shape,
        in_specs=[vm] * len(out_shape),
        out_specs=(hbm,) * len(out_shape),
        scratch_shapes=[dma((len(out_shape),))],
        compiler_params=pltpu.CompilerParams(vmem_limit_bytes=28 * 1024 * 1024),
    )(*outs)
    d_tokens, d_gates, gw, lw, dw, gn, ln, dn = outs
    return (d_tokens, d_gates.T, gw[None], lw[None], dw[None], gn, ln, dn)


def solution(mesh):
    in_specs = (
        P("ep", None),
        P("ep", None),
        P("ep", None),
        P("ep", None),
        P("ep", None, "tp"),
        P("ep", None, "tp"),
        P("ep", "tp", None),
    )
    out_specs = (
        P("ep", "tp"),
        P("ep", None),
        P("ep", None, "tp"),
        P("ep", None, "tp"),
        P("ep", "tp", None),
        P("ep", None),
        P("ep", None),
        P("ep", "tp"),
    )
    return jax.shard_map(shards, mesh=mesh, in_specs=in_specs, out_specs=out_specs, check_vma=False)
```
